512 devices in a mesh: fs: 64 (over z, y), tp: 8 (over x, core).
Axes of the slice: x: 4, y: 8, z: 8, core: 2. Of those that a mesh axis runs over, the one named last changes fastest.
Arguments:
- gate_pre: bfloat16 [32768, 3072], P('fs', 'tp'), may hold values from -6 to 6
- up_pre: bfloat16 [32768, 3072], P('fs', 'tp'), may hold values from -6 to 6
- cotangent: bfloat16 [32768, 2048], P('fs'), may hold values from -8 to 8
- gate_weight: bfloat16 [2048, 3072], P('fs', 'tp'), may hold values from -0.125 to 0.125
- up_weight: bfloat16 [2048, 3072], P('fs', 'tp'), may hold values from -0.125 to 0.125
- down_weight: bfloat16 [2048, 3072], P('fs', 'tp'), may hold values from -0.109375 to 0.109375
Outputs:
- grad_input: bfloat16 [32768, 2048], P('fs')
- grad_down: float32 [2048, 3072], P('fs', 'tp')
The draws below stay inside these ranges and needn't reach their ends.
All inputs are finite; a program needn't handle non-finite values.
Results may differ from the reference program's by a relative error of at most 0.014.
Values may be sent and summed in bfloat16 or wider, within the bound.
A program may use at most 64 MiB of HBM per device.

```python
import jax
import jax.numpy as jnp
from jax import lax

D = 2048
FF = 3072
TOKENS = 32768
N_TP = 8


def strengthened(result, stream_key, source, target, blocks, factor):
    def block_of(position):
        return (jnp.arange(result.shape[position]) // (result.shape[position] // blocks)).reshape((-1,) + (1,) * (result.ndim - 1 - position))

    one_side = jax.random.permutation(stream_key, blocks)[block_of(target)]
    far = (block_of(target) + blocks // 2) % blocks
    return jnp.where((block_of(source) == one_side) | (block_of(source) == far), factor * result, result)


def steps_of(stream_key, shape, pieces, smallest, top_value):
    factor_of, own = 1.0, jax.random.fold_in(stream_key, 6)
    for position, shards_of in pieces:
        heights = jnp.exp(jax.random.uniform(jax.random.fold_in(own, position), (shards_of,), jnp.float32, smallest / len(pieces), top_value / len(pieces)))
        factor_of = factor_of * jnp.repeat(heights, shape[position] // shards_of).reshape([-1 if axis == position else 1 for axis in range(len(shape))])
    return factor_of


def noise(rng, extent, scale, most, split=(), held_as=jnp.bfloat16):
    drawn = scale * jax.random.normal(rng, extent, jnp.float32)
    if split:
        drawn = drawn * steps_of(rng, extent, split, -0.22, 0.18)
    return jnp.clip(drawn, -most, most).astype(held_as)


def gaussian_with(rng, shape, scale, bound, pieces, heavy, dtype=jnp.bfloat16):
    drawn = scale * jax.random.normal(rng, shape, jnp.float32)
    if pieces:
        drawn = drawn * steps_of(rng, shape, pieces, -0.22, 0.18)
    return jnp.clip(strengthened(drawn, jax.random.fold_in(rng, 3), *heavy), -bound, bound).astype(dtype)


def setup_inputs(seed: int = 0) -> dict:
    arg_keys = jax.random.split(jax.random.key(seed), 7)
    gate_pre = noise(arg_keys[0], (TOKENS, FF), 1.0, 6.0, ((0, 64), (1, 8)))
    up_pre = noise(arg_keys[1], (TOKENS, FF), 1.0, 6.0, ((0, 64), (1, 8)))
    cotangent = gaussian_with(arg_keys[2], (TOKENS, D), 1.0, 8.0, ((0, 64),), (0, 1, 64, 4.0))
    gate_weight = noise(arg_keys[3], (D, FF), D ** -0.5, 0.125, ((0, 64), (1, 8)))
    up_weight = noise(arg_keys[4], (D, FF), D ** -0.5, 0.125, ((0, 64), (1, 8)))
    down_weight = noise(arg_keys[5], (D, FF), FF ** -0.5, 0.109375, ((0, 64), (1, 8)))
    return dict(gate_pre=gate_pre, up_pre=up_pre, cotangent=cotangent, gate_weight=gate_weight, up_weight=up_weight, down_weight=down_weight)


def reference(gate_pre, up_pre, cotangent, gate_weight, up_weight, down_weight):
    gate = gate_pre.astype(jnp.float32)
    upper = up_pre.astype(jnp.float32)
    sigma = jax.nn.sigmoid(gate)
    hidden = (gate * sigma * upper).astype(jnp.bfloat16)
    d_hidden = jnp.dot(cotangent, down_weight, preferred_element_type=jnp.float32)
    d_gate = (d_hidden * upper * sigma * (1.0 + gate * (1.0 - sigma))).astype(jnp.bfloat16)
    d_up = (d_hidden * gate * sigma).astype(jnp.bfloat16)
    grad_down = lax.dot_general(cotangent, hidden, (((0,), (0,)), ((), ())), preferred_element_type=jnp.float32)
    width = FF // N_TP
    total = jnp.zeros((cotangent.shape[0], D), jnp.float32)
    for block in range(N_TP):
        lower = block * width
        part = lax.dot_general(d_gate[:, lower:lower + width], gate_weight[:, lower:lower + width], (((1,), (1,)), ((), ())), preferred_element_type=jnp.float32)
        part = part + lax.dot_general(d_up[:, lower:lower + width], up_weight[:, lower:lower + width], (((1,), (1,)), ((), ())), preferred_element_type=jnp.float32)
        total = total + part.astype(jnp.bfloat16).astype(jnp.float32)
    return total.astype(jnp.bfloat16), grad_down
```

```python
import functools

import jax
import jax.numpy as jnp
from jax import lax
from jax.experimental import pallas as pl
from jax.experimental.pallas import tpu as pltpu
from jax.sharding import PartitionSpec as P

MESH = pl.DeviceIdType.MESH
f32, bf16 = jnp.float32, jnp.bfloat16
N = 8
X = 4
T, D, F = 512, 2048, 384
H = 16
A, B = 0, 1
DOWN, GATE, UP = 0, 1, 2
LONG = {DOWN: -1, GATE: 1, UP: -1}
RS_LONG = 1
LAGS = (1, 3, 5, 7, 9, 10)


def reach(m, sign):
    return 4 if LONG[m] == sign else 3


def rs_reach(sign):
    return 4 if RS_LONG == sign else 3


def chunk_order():
    order = [(A, 1, 0), (B, 1, 0)]
    for k in (1, 2, 3):
        order += [(r, s, k) for r in (A, B) for s in (1, -1)]
    return order + [(A, 1, 4), (B, 1, 4)]


def kernel(
    gate_hbm, up_hbm, cot_hbm, wd_hbm, wg_hbm, wu_hbm,
    ot_hbm, gd_ref,
    gate, up, cot, w, hid, fa, fb, dg, du, g, rs_out, rs_in, lt_tot, lt_out, lt_in,
    part, dr, xs, xr, ot,
    load_sem, out_sem, ssem, rsem,
):
    fs, tp = lax.axis_index("fs"), lax.axis_index("tp")
    z, y = fs // N, fs % N
    x, c = tp // 2, tp % 2
    keys, sends = {}, []

    def ring(i):
        return lax.rem(i + N, N)

    def xring(i):
        return lax.rem(i + X, X)

    def at(zz, yy):
        return {"fs": zz * N + yy, "tp": tp}

    def along(xx, cc):
        return {"fs": fs, "tp": xx * 2 + cc}

    partner = along(x, 1 - c)

    def sem_of(key):
        return keys.setdefault(key, len(keys))

    def send(src, dst, device, key):
        i = sem_of(key)
        d = pltpu.make_async_remote_copy(src, dst, ssem.at[i], rsem.at[i], device_id=device, device_id_type=MESH)
        d.start()
        sends.append(d)

    def recv(dst, key):
        i = sem_of(key)
        pltpu.make_async_remote_copy(dst, dst, ssem.at[i], rsem.at[i], device_id=partner, device_id_type=MESH).wait_recv()

    loads = [pltpu.make_async_copy(src, w.at[m, z, y], load_sem.at[m]) for m, src in enumerate((wd_hbm, wg_hbm, wu_hbm))]
    loads += [pltpu.make_async_copy(gate_hbm, gate, load_sem.at[3]), pltpu.make_async_copy(up_hbm, up, load_sem.at[4])]
    loads += [pltpu.make_async_copy(cot_hbm, cot, load_sem.at[5])]
    for copy in loads:
        copy.start()
    barrier = pltpu.get_barrier_semaphore()
    peers = [at(z, ring(y + o)) for o in range(1, N)] + [at(ring(z + o), y) for o in range(1, N)]
    peers += [along(xring(x + 1), c), along(xring(x - 1), c), partner]
    for peer in peers:
        pl.semaphore_signal(barrier, inc=1, device_id=peer, device_id_type=MESH)
    for m in range(3):
        loads[m].wait()
    pl.semaphore_wait(barrier, len(peers))

    def first_ref(m, r, o):
        return w.at[m, z, ring(y + o), pl.ds(0, H)] if r == A else w.at[m, ring(z + o), y, pl.ds(H, H)]

    def first_send(m):
        for o in (4, 3, 5, 2, 6, 1, 7):
            for r in (A, B):
                ref = first_ref(m, r, 0)
                send(ref, ref, at(z, ring(y + o)) if r == A else at(ring(z + o), y), ("p1", m, r, o))

    def first_wait(m):
        for o in (1, 7, 2, 6, 3, 5, 4):
            for r in (A, B):
                recv(first_ref(m, r, -o), ("p1", m, r, o))

    def group(m, r, i):
        return w.at[m, ring(z + i), :, pl.ds(0, H)] if r == A else w.at[m, :, ring(y + i), pl.ds(H, H)]

    def second_send(m, r, s, k):
        if k > reach(m, s):
            return
        ref = group(m, r, -s * (k - 1))
        send(ref, ref, at(ring(z + s), y) if r == A else at(z, ring(y + s)), ("p2", m, r, s, k))

    def second_recv(m, r, s, k):
        if k <= reach(m, s):
            recv(group(m, r, -s * k), ("p2", m, r, s, k))

    ALL = [(r, s) for r in (A, B) for s in (1, -1)]

    for m in (DOWN, GATE, UP):
        first_send(m)

    loads[3].wait()
    loads[4].wait()

    @pl.loop(0, T // 64)
    def _(i):
        rows = pl.ds(pl.multiple_of(i * 64, 64), 64)
        gv, uv = gate[rows].astype(f32), up[rows].astype(f32)
        sv = jax.nn.sigmoid(gv)
        gs = gv * sv
        hid[rows] = (gs * uv).astype(bf16)
        fa[rows] = uv * sv * (1.0 + gv * (1.0 - sv))
        fb[rows] = gs

    loads[5].wait()

    @pl.loop(0, N)
    def _(i):
        columns = pl.ds(pl.multiple_of(i * 256, 256), 256)
        block = lax.dot_general(cot[:, columns], hid[...], (((0,), (0,)), ((), ())), preferred_element_type=f32)
        g[i] = block.reshape(N, 2 * H, F)

    def own(r, i):
        return g[:, ring(y + i), pl.ds(0, H)] if r == A else g[ring(z + i), :, pl.ds(H, H)]

    def slot(s, k):
        return (0 if s == 1 else 4) + k - 1

    def rs_send(r, s, k):
        if k > rs_reach(s):
            return
        value = own(r, s * (rs_reach(s) - k + 1))
        if k > 1:
            value = value + rs_in[r, slot(s, k - 1)].astype(f32)
        rs_out[r, slot(s, k)] = value.astype(bf16)
        device = at(z, ring(y + s)) if r == A else at(ring(z + s), y)
        send(rs_out.at[r, slot(s, k)], rs_in.at[r, slot(s, k)], device, ("rs", r, s, k))

    def rs_recv(r, s, k):
        if k <= rs_reach(s):
            recv(rs_in.at[r, slot(s, k)], ("rs", r, s, k))

    def light_send(r):
        total = own(r, 0) + rs_in[r, slot(1, rs_reach(1))].astype(f32) + rs_in[r, slot(-1, rs_reach(-1))].astype(f32)
        lt_tot[r] = total
        lt_out[r] = total.astype(bf16)
        me = z if r == A else y
        for o in (4, 3, 5, 2, 6, 1, 7):
            device = at(ring(z + o), y) if r == A else at(z, ring(y + o))
            send(lt_out.at[r, ring(me + o)], lt_in.at[r, me], device, ("lt", r, o))

    def light_finish(r):
        me = z if r == A else y
        total = lt_tot[r, me]
        for o in range(1, N):
            recv(lt_in.at[r, ring(me - o)], ("lt", r, o))
            total = total + lt_in[r, ring(me - o)].astype(f32)
        gd_ref[pl.ds(r * H, H)] = total

    first_wait(DOWN)
    for r, s in ALL:
        second_send(DOWN, r, s, 1)
    for r, s in ALL:
        rs_send(r, s, 1)
    first_wait(GATE)
    first_wait(UP)
    for k in (1, 2, 3, 4):
        for r, s in ALL:
            second_recv(DOWN, r, s, k)
            second_send(DOWN, r, s, k + 1)
        for r, s in ALL:
            rs_recv(r, s, k)
            rs_send(r, s, k + 1)
        if k == 2:
            for r, s in ALL:
                second_send(GATE, r, s, 1)
        if k == 3:
            for r, s in ALL:
                second_send(UP, r, s, 1)

    d_hidden = jnp.dot(cot[...], w[DOWN].reshape(D, F), preferred_element_type=f32)
    dg[...] = (d_hidden * fa[...]).astype(bf16)
    du[...] = (d_hidden * fb[...]).astype(bf16)
    for r in (A, B):
        light_send(r)

    order = chunk_order()
    outs = []

    def way(i):
        return 1 if i % 2 == 0 else -1

    def piece(i, q, n=None):
        r, s, k = order[i]
        q = q if n is None else pl.ds(q, n)
        if r == A:
            return ot.at[ring(z - s * k), q, pl.ds(0, H)]
        return ot.at[q, ring(y - s * k), pl.ds(H, H)]

    def arrive(i):
        r, s, k = order[i]
        if k == 0:
            return
        for m in (GATE, UP):
            for ss in (1, -1) if k == 4 else (s,):
                second_recv(m, r, ss, k)
                second_send(m, r, ss, k + 1)

    def sums(i, j):
        return part[i, c * X + j].astype(f32) + dr[i, j].astype(f32)

    def stage0(i):
        r, s, k = order[i]
        arrive(i)

        def rows_of(m):
            v = w[m, ring(z - s * k), :, pl.ds(0, H)] if r == A else w[m, :, ring(y - s * k), pl.ds(H, H)]
            return v.reshape(N * H, F)

        nt = (((1,), (1,)), ((), ()))
        p = lax.dot_general(rows_of(GATE), dg[...], nt, preferred_element_type=f32)
        p = p + lax.dot_general(rows_of(UP), du[...], nt, preferred_element_type=f32)
        part[i] = p.astype(bf16).reshape(N, H, T)
        send(part.at[i, pl.ds((1 - c) * X, X)], dr.at[i], partner, ("d2d", i))

    def stage1(i):
        s = way(i)
        recv(dr.at[i], ("d2d", i))
        xs[i, 0] = sums(i, xring(x + 2)).astype(bf16)
        send(xs.at[i, 0], xr.at[i, 0], along(xring(x + s), c), ("x1", i))
        xs[i, 1] = sums(i, xring(x - s)).astype(bf16)
        send(xs.at[i, 1], xr.at[i, 1], along(xring(x - s), c), ("x2", i))

    def stage2(i):
        s = way(i)
        recv(xr.at[i, 0], ("x1", i))
        xs[i, 2] = (sums(i, xring(x + s)) + xr[i, 0].astype(f32)).astype(bf16)
        send(xs.at[i, 2], xr.at[i, 2], along(xring(x + s), c), ("x3", i))

    def stage3(i):
        recv(xr.at[i, 1], ("x2", i))
        recv(xr.at[i, 2], ("x3", i))
        total = sums(i, x) + xr[i, 1].astype(f32) + xr[i, 2].astype(f32)
        mine = piece(i, c * X + x)
        mine[...] = total.astype(bf16)
        for s in (1, -1):
            send(mine, mine, along(xring(x + s), c), ("g1", i, s))

    def stage4(i):
        s = way(i)
        behind = piece(i, c * X + xring(x - s))
        recv(behind, ("g1", i, s))
        send(behind, behind, along(xring(x + s), c), ("g2", i))
        recv(piece(i, c * X + xring(x + s)), ("g1", i, -s))

    def stage5(i):
        recv(piece(i, c * X + xring(x + 2)), ("g2", i))
        half = piece(i, c * X, X)
        send(half, half, partner, ("g3", i))

    def stage6(i):
        recv(piece(i, (1 - c) * X, X), ("g3", i))
        r, s, k = order[i]
        if r == A:
            src, dst = (ref.at[ring(z - s * k), :, pl.ds(0, H)] for ref in (ot, ot_hbm))
        else:
            src, dst = (ref.at[:, ring(y - s * k), pl.ds(H, H)] for ref in (ot, ot_hbm))
        copy = pltpu.make_async_copy(src, dst, out_sem.at[i])
        copy.start()
        outs.append(copy)

    stages = (stage1, stage2, stage3, stage4, stage5, stage6)
    chunks = len(order)
    for i in range(chunks + LAGS[-1]):
        for lag, stage in reversed(list(zip(LAGS, stages))):
            if 0 <= i - lag < chunks:
                stage(i - lag)
        if i < chunks:
            stage0(i)
        if i == 8:
            for r in (A, B):
                light_finish(r)

    for d in sends:
        d.wait_send()
    for copy in outs:
        copy.wait()


SEMS = 240


def local(gate_pre, up_pre, cotangent, gate_weight, up_weight, down_weight):
    hbm = pl.BlockSpec(memory_space=pltpu.HBM)
    ot, grad_down = pl.pallas_call(
        kernel,
        out_shape=(jax.ShapeDtypeStruct((N, N, 2 * H, T), bf16), jax.ShapeDtypeStruct((2 * H, F), f32)),
        in_specs=[hbm] * 6,
        out_specs=(hbm, pl.BlockSpec(memory_space=pltpu.VMEM)),
        scratch_shapes=[
            pltpu.VMEM((T, F), bf16),
            pltpu.VMEM((T, F), bf16),
            pltpu.VMEM((T, D), bf16),
            pltpu.VMEM((3, N, N, 2 * H, F), bf16),
            pltpu.VMEM((T, F), bf16),
            pltpu.VMEM((T, F), f32),
            pltpu.VMEM((T, F), f32),
            pltpu.VMEM((T, F), bf16),
            pltpu.VMEM((T, F), bf16),
            pltpu.VMEM((N, N, 2 * H, F), f32),
            pltpu.VMEM((2, 7, N, H, F), bf16),
            pltpu.VMEM((2, 7, N, H, F), bf16),
            pltpu.VMEM((2, N, H, F), f32),
            pltpu.VMEM((2, N, H, F), bf16),
            pltpu.VMEM((2, N, H, F), bf16),
            pltpu.VMEM((16, N, H, T), bf16),
            pltpu.VMEM((16, X, H, T), bf16),
            pltpu.VMEM((16, 3, H, T), bf16),
            pltpu.VMEM((16, 3, H, T), bf16),
            pltpu.VMEM((N, N, 2 * H, T), bf16),
            pltpu.SemaphoreType.DMA((6,)),
            pltpu.SemaphoreType.DMA((16,)),
            pltpu.SemaphoreType.DMA((SEMS,)),
            pltpu.SemaphoreType.DMA((SEMS,)),
        ],
        compiler_params=pltpu.CompilerParams(
            collective_id=0, has_side_effects=True, vmem_limit_bytes=60 * 1024 * 1024
        ),
    )(gate_pre, up_pre, cotangent, down_weight, gate_weight, up_weight)
    return ot.reshape(D, T).T, grad_down


def solution(mesh):
    placed = (P("fs", "tp"), P("fs", "tp"), P("fs", None), P("fs", "tp"), P("fs", "tp"), P("fs", "tp"))
    return jax.shard_map(
        local, mesh=mesh, in_specs=placed, out_specs=(P("fs", None), P("fs", "tp")), check_vma=False
    )
```
